32 devices in a mesh: fs: 4 (over z), rep: 4 (over y, x), tp: 2 (over core).
Axes of the slice: x: 2, y: 2, z: 4, core: 2. Of those that a mesh axis runs over, the one named last changes fastest.
Arguments:
- saved_input: bfloat16 [32768, 2048], P(('fs', 'rep')), may hold values from -8 to 8
- query_cotangent: bfloat16 [32768, 1024], P(('fs', 'rep'), 'tp'), may hold values from -0.03125 to 0.03125
- saved_heads: bfloat16 [32768, 1024], P(('fs', 'rep'), 'tp'), may hold values from -6 to 6
- block_cotangent: bfloat16 [32768, 2048], P(('fs', 'rep')), may hold values from -0.046875 to 0.046875
- query_weight: float32 [2048, 1024], P(('fs', 'rep'), 'tp'), may hold values from -6 to 6
- output_weight: float32 [1024, 2048], P('tp', ('fs', 'rep')), may hold values from -6 to 6
- query_factor: bfloat16 [2048, 256], P(('fs', 'rep')), may hold values from -0.125 to 0.125
- output_factor: bfloat16 [2048, 256], P(('fs', 'rep')), may hold values from -0.125 to 0.125
- query_first: float32 [256, 1024], P(None, 'tp'), may hold values from -6 to 6
- query_second: float32 [256, 1024], P(None, 'tp'), may hold values from 0.5 to 2
- output_first: float32 [1024, 256], P('tp'), may hold values from -6 to 6
- output_second: float32 [1024, 256], P('tp'), may hold values from 0.5 to 2
Outputs:
- new_query_weight: float32 [2048, 1024], P(('fs', 'rep'), 'tp')
- new_output_weight: float32 [1024, 2048], P('tp', ('fs', 'rep'))
- new_query_first: float32 [256, 1024], P(None, 'tp')
- new_query_second: float32 [256, 1024], P(None, 'tp')
- new_output_first: float32 [1024, 256], P('tp')
- new_output_second: float32 [1024, 256], P('tp')
- query_step: float32 [2048, 1024], P(('fs', 'rep'), 'tp')
- output_step: float32 [1024, 2048], P('tp', ('fs', 'rep'))
- query_copy: bfloat16 [2048, 1024], P(None, 'tp')
- output_copy: bfloat16 [1024, 2048], P('tp')
The draws below stay inside these ranges and needn't reach their ends.
All inputs are finite; a program needn't handle non-finite values.
Results may differ from the reference program's by a relative error of at most 0.0013.
Values may be sent and summed in bfloat16 or wider, within the bound.
A program may use at most 128 MiB of HBM per device.

```python
import math
import jax
import jax.numpy as jnp
from jax import lax

D = 2048
RANK = 256
SBW = 1024
TOKENS = 32768


def strengthened(array, own_key, source, target, shards_of, factor):
    owner, partner = [(jnp.arange(array.shape[axis_at]) // (array.shape[axis_at] // shards_of)).reshape([-1 if axis == axis_at else 1 for axis in range(array.ndim)]) for axis_at in (source, target)]
    chosen = jax.random.permutation(own_key, shards_of)[partner]
    strong = (owner == chosen) | (owner == (partner + shards_of // 2) % shards_of)
    return jnp.where(strong, factor * array, array)


def block_levels(rng, shape, pieces, least, top_value):
    def one(position, shards_of):
        heights = jax.random.uniform(jax.random.fold_in(jax.random.fold_in(rng, 6), position), (shards_of,), jnp.float32, least / len(pieces), top_value / len(pieces))
        return jnp.repeat(jnp.exp(heights), shape[position] // shards_of).reshape((-1,) + (1,) * (len(shape) - position - 1))

    level = one(*pieces[0])
    for cut in pieces[1:]:
        level = level * one(*cut)
    return level


def normal_values(rng, extent, deviation, bound, cuts=(), dtype=jnp.bfloat16):
    entries = deviation * jax.random.normal(rng, extent, jnp.float32)
    if cuts:
        entries = entries * block_levels(rng, extent, cuts, -0.22, 0.18)
    return jnp.clip(entries, -bound, bound).astype(dtype)


def noise_with(rng, shape, deviation, bound, split, heavy, kind=jnp.bfloat16):
    drawn = deviation * jax.random.normal(rng, shape, jnp.float32)
    if split:
        drawn = drawn * block_levels(rng, shape, split, -0.22, 0.18)
    return jnp.clip(strengthened(drawn, jax.random.fold_in(rng, 3), *heavy), -bound, bound).astype(kind)


def setup_inputs(seed: int = 0) -> dict:
    arg_keys = jax.random.split(jax.random.key(seed), 13)
    return {
        "saved_input": noise_with(arg_keys[0], (TOKENS, D), 1.0, 8.0, ((0, 16),), (0, 1, 16, 2.0)),
        "query_cotangent": normal_values(arg_keys[1], (TOKENS, SBW), (TOKENS ** -0.5), 0.03125, ((0, 16), (1, 2))),
        "saved_heads": normal_values(arg_keys[2], (TOKENS, SBW), 1.0, 6.0, ((0, 16), (1, 2))),
        "block_cotangent": noise_with(arg_keys[3], (TOKENS, D), (TOKENS ** -0.5), 0.046875, ((0, 16),), (0, 1, 16, 2.0)),
        "query_weight": normal_values(arg_keys[4], (D, SBW), 1.0, 6.0, ((0, 16), (1, 2)), jnp.float32),
        "output_weight": normal_values(arg_keys[5], (SBW, D), 1.0, 6.0, ((0, 2), (1, 16)), jnp.float32),
        "query_factor": normal_values(arg_keys[6], (D, RANK), D ** -0.5, 0.125, ((0, 16),)),
        "output_factor": normal_values(arg_keys[7], (D, RANK), D ** -0.5, 0.125, ((0, 16),)),
        "query_first": normal_values(arg_keys[8], (RANK, SBW), 1.0, 6.0, ((1, 2),), jnp.float32),
        "query_second": jnp.clip(jnp.exp(math.log(2.0) - 1.3862944 * jax.random.uniform(arg_keys[9], (RANK, SBW), jnp.float32) ** block_levels(arg_keys[9], (RANK, SBW), ((1, 2),), -0.2, 0.2)), 0.5, 2.0),
        "output_first": normal_values(arg_keys[10], (SBW, RANK), 1.0, 6.0, ((0, 2),), jnp.float32),
        "output_second": jnp.clip(jnp.exp(math.log(2.0) - 1.3862944 * jax.random.uniform(arg_keys[11], (SBW, RANK), jnp.float32) ** block_levels(arg_keys[11], (SBW, RANK), ((0, 2),), -0.2, 0.2)), 0.5, 2.0),
    }


def reference(saved_input, query_cotangent, saved_heads, block_cotangent, query_weight, output_weight, query_factor, output_factor, query_first, query_second, output_first, output_second):
    contract = (((0,), (0,)), ((), ()))
    high = lax.Precision.HIGHEST
    query_grad = lax.dot_general(saved_input, query_cotangent, contract, preferred_element_type=jnp.float32)
    output_grad = lax.dot_general(saved_heads, block_cotangent, contract, preferred_element_type=jnp.float32)
    factor_q = query_factor.astype(jnp.float32)
    factor_o = output_factor.astype(jnp.float32)
    query_proj = jnp.dot(factor_q.T, query_grad, precision=high)
    output_proj = jnp.dot(output_grad, factor_o, precision=high)
    new_query_first = 0.9 * query_first + 0.1 * query_proj
    new_output_first = 0.9 * output_first + 0.1 * output_proj
    new_query_second = 0.95 * query_second + 0.05 * query_proj * query_proj
    new_output_second = 0.95 * output_second + 0.05 * output_proj * output_proj
    query_dir = new_query_first / (jnp.sqrt(new_query_second) + 1e-08)
    output_dir = new_output_first / (jnp.sqrt(new_output_second) + 1e-08)
    query_raw = jnp.dot(factor_q, query_dir, precision=high)
    output_raw = jnp.dot(output_dir, factor_o.T, precision=high)
    query_step = query_raw / jnp.sqrt(jnp.mean(query_raw * query_raw) + 0.01)
    output_step = output_raw / jnp.sqrt(jnp.mean(output_raw * output_raw) + 0.01)
    new_query_weight = query_weight - 0.1 * query_step
    new_output_weight = output_weight - 0.1 * output_step
    return (new_query_weight, new_output_weight, new_query_first, new_query_second, new_output_first, new_output_second, query_step, output_step, new_query_weight.astype(jnp.bfloat16), new_output_weight.astype(jnp.bfloat16))
```

```python
import functools

import jax
import jax.numpy as jnp
from jax import lax
from jax.experimental import pallas as pl
from jax.experimental.pallas import tpu as pltpu
from jax.sharding import PartitionSpec as P

MESH = pl.DeviceIdType.MESH
BF = jnp.bfloat16
F32 = jnp.float32


def split_parts(wide):
    upper = wide.astype(BF)
    lower = (wide - upper.astype(F32)).astype(BF)
    return (upper, lower)


def remote(src, dst, send, recv, where):
    copy = pltpu.make_async_remote_copy(
        src_ref=src, dst_ref=dst, send_sem=send, recv_sem=recv, device_id=where, device_id_type=MESH
    )
    return copy


def place(nf, nr):
    f, r, t = lax.axis_index("fs"), lax.axis_index("rep"), lax.axis_index("tp")
    near = r + 1 - 2 * lax.rem(r, 2)
    side = lax.rem(r + 2, 4)
    far = 3 - r
    return f, r, t, near, side, far


def greet(nf, f, near, side, far, t):
    barrier = pltpu.get_barrier_semaphore()
    for df in range(1, nf):
        pl.semaphore_signal(barrier, inc=1, device_id={"fs": lax.rem(f + df, nf)}, device_id_type=MESH)
    for peer in (near, side, far):
        pl.semaphore_signal(barrier, inc=1, device_id={"rep": peer}, device_id_type=MESH)
    pl.semaphore_signal(barrier, inc=1, device_id={"tp": 1 - t}, device_id_type=MESH)
    pl.semaphore_wait(barrier, nf - 1 + 4)


def gather(nf, nr, f, r, near, side, far, parts, first, second, sems, passed=None):
    fs_s, fs_r, n_s, n_r, s_s, s_r, d_s, d_r = sems
    width = len(parts(0))
    half = len(first(0))
    me = f * nr + r
    sent = []

    def send(refs, send_sem, recv_sem, row, where):
        got = []
        for k, ref in enumerate(refs):
            copy = remote(ref, ref, send_sem.at[row, k], recv_sem.at[row, k], where)
            copy.start()
            got.append(copy)
        sent.extend(got)

    def arrive(refs, send_sem, recv_sem, row, where):
        for k, ref in enumerate(refs):
            remote(ref, ref, send_sem.at[row, k], recv_sem.at[row, k], where).wait_recv()

    send(parts(me), n_s, n_r, 0, {"rep": near})
    send(parts(me), s_s, s_r, 0, {"rep": side})
    for df in range(1, nf):
        send(parts(me), fs_s, fs_r, df, {"fs": lax.rem(f + df, nf)})
    for df in range(nf):
        from_f = lax.rem(f + nf - df, nf)
        if df > 0:
            slot = from_f * nr + r
            arrive(parts(slot), fs_s, fs_r, df, {"fs": from_f})
            send(parts(slot), n_s, n_r, df, {"rep": near})
            send(parts(slot), s_s, s_r, df, {"rep": side})
            if passed:
                passed(slot)
        if df > 0:
            relay(nf, nr, f, near, side, df - 1, parts, first, second, arrive, send, sems, passed)
    relay(nf, nr, f, near, side, nf - 1, parts, first, second, arrive, send, sems, passed)
    for df in range(nf):
        slot = lax.rem(f + nf - df, nf) * nr + far
        arrive(first(slot), d_s.at[0], d_r.at[0], df, {"rep": side})
        arrive(second(slot), d_s.at[1], d_r.at[1], df, {"rep": near})
        if passed:
            passed(slot)
    for copy in sent:
        copy.wait_send()


def relay(nf, nr, f, near, side, df, parts, first, second, arrive, send, sems, passed):
    fs_s, fs_r, n_s, n_r, s_s, s_r, d_s, d_r = sems
    from_f = lax.rem(f + nf - df, nf)
    one = from_f * nr + near
    arrive(parts(one), n_s, n_r, df, {"rep": near})
    send(first(one), d_s.at[0], d_r.at[0], df, {"rep": side})
    two = from_f * nr + side
    arrive(parts(two), s_s, s_r, df, {"rep": side})
    send(second(two), d_s.at[1], d_r.at[1], df, {"rep": near})
    if passed:
        passed(one)
        passed(two)


def gather_sems(nf, width, half):
    dma = pltpu.SemaphoreType.DMA
    return [dma((nf, width))] * 6 + [dma((2, nf, half))] * 2


def factor_kernel(nf, nr, fq_ref, fo_ref, out_ref, *sems):
    f, r, t, near, side, far = place(nf, nr)
    local, p_s, p_r = sems[8:]
    me = f * nr + r
    rows = fq_ref.shape[0]
    copies = [
        pltpu.make_async_copy(fq_ref, out_ref.at[0, me], local.at[0]),
        pltpu.make_async_copy(fo_ref, out_ref.at[1, me], local.at[1]),
    ]
    for copy in copies:
        copy.start()
    greet(nf, f, near, side, far, t)
    for copy in copies:
        copy.wait()
    relayed = []

    def passed(slot):
        copy = remote(
            out_ref.at[t, slot], out_ref.at[t, slot], p_s.at[len(relayed)], p_r.at[len(relayed)], {"tp": 1 - t}
        )
        copy.start()
        relayed.append(slot)

    gather(
        nf, nr, f, r, near, side, far,
        lambda s: [out_ref.at[t, s]],
        lambda s: [out_ref.at[t, s, pl.ds(0, rows // 2)]],
        lambda s: [out_ref.at[t, s, pl.ds(rows // 2, rows // 2)]],
        sems[:8],
        passed,
    )
    for k, slot in enumerate(relayed):
        copy = remote(out_ref.at[t, slot], out_ref.at[t, slot], p_s.at[k], p_r.at[k], {"tp": 1 - t})
        copy.wait_send()
        remote(out_ref.at[1 - t, slot], out_ref.at[1 - t, slot], p_s.at[k], p_r.at[k], {"tp": 1 - t}).wait_recv()


def update_kernel(
    nf, nr, wide,
    part_ref, factor_ref, wq_ref, wo_ref, fq_ref, sq_ref, fo_ref, so_ref,
    nwq_ref, nwo_ref, nfq_ref, nsq_ref, nfo_ref, nso_ref, stq_ref, sto_ref, cq_ref, co_ref,
    outgoing, landed, partial, exchanged, whole, dirs, square, *sems,
):
    f, r, t, near, side, far = place(nf, nr)
    a_s, a_r, b_s, b_r, c_s, c_r, e_s, e_r, x_s, x_r = sems[8:]
    n = nf * nr
    me = f * nr + r
    depth = factor_ref.shape[2]
    rank = dirs.shape[2]
    for k in range(nr):
        outgoing[k] = part_ref[k].astype(BF)
    greet(nf, f, near, side, far, t)
    sent = []
    peers = (near, side, far)
    for k, peer in enumerate(peers):
        copy = remote(outgoing.at[peer], landed.at[k], a_s.at[k], a_r.at[k], {"rep": peer})
        copy.start()
        sent.append(copy)
    for k, peer in enumerate(peers):
        remote(outgoing.at[peer], landed.at[k], a_s.at[k], a_r.at[k], {"rep": peer}).wait_recv()
    total = part_ref[r] + landed[0].astype(F32) + landed[1].astype(F32) + landed[2].astype(F32)
    partial[...] = total.astype(BF)
    for df in range(1, nf):
        to = lax.rem(f + df, nf)
        copy = remote(partial.at[to], exchanged.at[df], b_s.at[df], b_r.at[df], {"fs": to})
        copy.start()
        sent.append(copy)
    mine = part_ref[r, f] + landed[0, f].astype(F32) + landed[1, f].astype(F32) + landed[2, f].astype(F32)
    for df in range(1, nf):
        remote(partial.at[f], exchanged.at[df], b_s.at[df], b_r.at[df], {"fs": f}).wait_recv()
        mine = mine + exchanged[df].astype(F32)
    whole[r, f] = mine.astype(BF)
    for df in range(nf):
        from_f = lax.rem(f + nf - df, nf)
        if df == 0:
            for step in range(1, nf):
                copy = remote(
                    whole.at[r, f], whole.at[r, f], c_s.at[step], c_r.at[step], {"fs": lax.rem(f + step, nf)}
                )
                copy.start()
                sent.append(copy)
        else:
            ref = whole.at[r, from_f]
            remote(ref, ref, c_s.at[df], c_r.at[df], {"fs": from_f}).wait_recv()
        for k, peer in enumerate(peers):
            ref = whole.at[r, from_f]
            copy = remote(ref, ref, e_s.at[k, df], e_r.at[k, df], {"rep": peer})
            copy.start()
            sent.append(copy)
    for df in range(nf):
        from_f = lax.rem(f + nf - df, nf)
        for k, peer in enumerate(peers):
            ref = whole.at[peer, from_f]
            remote(ref, ref, e_s.at[k, df], e_r.at[k, df], {"rep": peer}).wait_recv()
    rows = nr // 2
    cols = part_ref.shape[3]
    for which, first, second, new_first, new_second in (
        (0, fq_ref, sq_ref, nfq_ref, nsq_ref),
        (1, fo_ref, so_ref, nfo_ref, nso_ref),
    ):
        proj = whole[which * rows : (which + 1) * rows].astype(F32).reshape(rank, cols)
        if which:
            proj = proj.T
        moved = 0.9 * first[...] + 0.1 * proj
        spread = 0.95 * second[...] + 0.05 * proj * proj
        new_first[...] = moved
        new_second[...] = spread
        way = moved / (jnp.sqrt(spread) + 1e-08)
        if which:
            way = way.T
        upper, lower = split_parts(way)
        dirs[which, 0] = upper
        dirs[which, 1] = lower

    def raw_of(which, slot):
        block = factor_ref[which, slot]
        return jnp.dot(block, dirs[which, 0], preferred_element_type=F32) + jnp.dot(
            block, dirs[which, 1], preferred_element_type=F32
        )

    for which in range(2):
        def add(slot, carry):
            raw = raw_of(which, slot)
            return carry + jnp.sum((raw * raw).reshape(depth // 8, 8, cols), axis=0)

        tally = lax.fori_loop(0, n, add, jnp.zeros((8, cols), F32))
        square[0, which] = tally
    copy = remote(square.at[0], square.at[1], x_s, x_r, {"tp": 1 - t})
    copy.start()
    raw_q = raw_of(0, me)
    raw_o = raw_of(1, me).T
    copy.wait()
    entries = wide * cols * 2
    sums = [
        jnp.sum(square[0, which] + square[1, which]) / entries + 0.01 for which in range(2)
    ]
    for raw, mean, weight, new_weight, step_ref, which in (
        (raw_q, sums[0], wq_ref, nwq_ref, stq_ref, 0),
        (raw_o, sums[1], wo_ref, nwo_ref, sto_ref, 1),
    ):
        step = raw / jnp.sqrt(jnp.full(raw.shape, mean, F32))
        new = weight[...] - 0.1 * step
        step_ref[...] = step
        new_weight[...] = new
        if which == 0:
            cq_ref[me] = new.astype(BF)
        elif depth % 128 == 0:
            co_ref[:, pl.ds(pl.multiple_of(me * depth, 128), depth)] = new.astype(BF)
        else:
            co_ref[me] = new.astype(BF)

    def output_slot(slot):
        if depth % 128 == 0:
            return co_ref.at[:, pl.ds(pl.multiple_of(slot * depth, 128), depth)]
        return co_ref.at[slot]

    gather(
        nf, nr, f, r, near, side, far,
        lambda s: [cq_ref.at[s], output_slot(s)],
        lambda s: [cq_ref.at[s]],
        lambda s: [output_slot(s)],
        sems[:8],
    )
    for copy in sent:
        copy.wait_send()


def body(
    nf, nr,
    saved_input, query_cotangent, saved_heads, block_cotangent, query_weight, output_weight,
    query_factor, output_factor, query_first, query_second, output_first, output_second,
):
    contract = (((0,), (0,)), ((), ()))
    n = nf * nr
    depth, rank = query_factor.shape
    cols = query_weight.shape[1]
    dma = pltpu.SemaphoreType.DMA
    vmem = pl.BlockSpec(memory_space=pltpu.VMEM)
    factors = pl.pallas_call(
        functools.partial(factor_kernel, nf, nr),
        out_shape=jax.ShapeDtypeStruct((2, n, depth, rank), BF),
        in_specs=[vmem] * 2,
        out_specs=vmem,
        scratch_shapes=gather_sems(nf, 1, 1) + [dma((2,)), dma((n,)), dma((n,))],
        compiler_params=pltpu.CompilerParams(collective_id=0, has_side_effects=True),
    )(query_factor, output_factor)
    whole_q = factors[0].reshape(n * depth, rank)
    whole_o = factors[1].reshape(n * depth, rank)
    input_low = jnp.dot(saved_input, whole_q, preferred_element_type=F32)
    cotan_low = jnp.dot(block_cotangent, whole_o, preferred_element_type=F32)
    input_upper, input_lower = split_parts(input_low)
    cotan_upper, cotan_lower = split_parts(cotan_low)
    part_query = lax.dot_general(
        input_upper, query_cotangent, contract, preferred_element_type=F32
    ) + lax.dot_general(input_lower, query_cotangent, contract, preferred_element_type=F32)
    part_output = lax.dot_general(
        cotan_upper, saved_heads, contract, preferred_element_type=F32
    ) + lax.dot_general(cotan_lower, saved_heads, contract, preferred_element_type=F32)
    rows = 2 * rank // n
    part = jnp.concatenate([part_query, part_output], axis=0).reshape(nr, nf, rows, cols)
    aligned = depth % 128 == 0
    shape = jax.ShapeDtypeStruct
    outs = pl.pallas_call(
        functools.partial(update_kernel, nf, nr, n * depth),
        out_shape=[
            shape((depth, cols), F32), shape((cols, depth), F32),
            shape((rank, cols), F32), shape((rank, cols), F32),
            shape((cols, rank), F32), shape((cols, rank), F32),
            shape((depth, cols), F32), shape((cols, depth), F32),
            shape((n, depth, cols), BF),
            shape((cols, n * depth) if aligned else (n, cols, depth), BF),
        ],
        in_specs=[vmem] * 8,
        out_specs=[vmem] * 10,
        scratch_shapes=[
            pltpu.VMEM((nr, nf, rows, cols), BF),
            pltpu.VMEM((3, nf, rows, cols), BF),
            pltpu.VMEM((nf, rows, cols), BF),
            pltpu.VMEM((nf, rows, cols), BF),
            pltpu.VMEM((nr, nf, rows, cols), BF),
            pltpu.VMEM((2, 2, rank, cols), BF),
            pltpu.VMEM((2, 2, 8, cols), F32),
        ]
        + gather_sems(nf, 2, 1)
        + [dma((3,)), dma((3,)), dma((nf,)), dma((nf,)), dma((nf,)), dma((nf,)), dma((3, nf)), dma((3, nf)), dma, dma],
        compiler_params=pltpu.CompilerParams(
            collective_id=1, has_side_effects=True, vmem_limit_bytes=60 * 1024 * 1024
        ),
    )(part, factors, query_weight, output_weight, query_first, query_second, output_first, output_second)
    *rest, query_copy, output_copy = outs
    query_copy = query_copy.reshape(n * depth, cols)
    if not aligned:
        output_copy = output_copy.transpose(1, 0, 2).reshape(cols, n * depth)
    return (*rest, query_copy, output_copy)


def solution(mesh):
    nf, nr = mesh.shape["fs"], mesh.shape["rep"]
    in_specs = (
        P(("fs", "rep"), None), P(("fs", "rep"), "tp"), P(("fs", "rep"), "tp"), P(("fs", "rep"), None),
        P(("fs", "rep"), "tp"), P("tp", ("fs", "rep")), P(("fs", "rep"), None), P(("fs", "rep"), None),
        P(None, "tp"), P(None, "tp"), P("tp", None), P("tp", None),
    )
    out_specs = (
        P(("fs", "rep"), "tp"), P("tp", ("fs", "rep")), P(None, "tp"), P(None, "tp"), P("tp", None), P("tp", None),
        P(("fs", "rep"), "tp"), P("tp", ("fs", "rep")), P(None, "tp"), P("tp", None),
    )
    return jax.shard_map(
        functools.partial(body, nf, nr), mesh=mesh, in_specs=in_specs, out_specs=out_specs, check_vma=False
    )
```
